32 devices in a mesh: sp: 16 (over z, x, core), tp: 2 (over y).
Axes of the slice: x: 2, y: 2, z: 4, core: 2. Of those that a mesh axis runs over, the one named last changes fastest.
Arguments:
- moe_input: bfloat16 [4096, 2048], P('sp'), may hold values from -6 to 6
- out_grad: bfloat16 [4096, 2048], P('sp'), may hold values from -0.29882812 to 0.29882812
- route_ids: int32 [4096, 2], P('sp'), may hold values from 0 to 15, all different within a row; in each aligned block of 256 rows (0 to 255, 256 to 511, ...) at most 40 rows name the same one
- route_weights: float32 [4096, 2], P('sp'), may hold values from 0.2 to 1
- gate_weight: bfloat16 [16, 1024, 2048], P('sp', 'tp'), may hold values from -0.1875 to 0.1875
- lin_weight: bfloat16 [16, 1024, 2048], P('sp', 'tp'), may hold values from -0.1875 to 0.1875
- down_weight: bfloat16 [16, 1024, 2048], P('sp', 'tp'), may hold values from -0.1875 to 0.1875
- outer_gate: bfloat16 [4096, 2048], P('sp', 'tp'), may hold values from -6 to 6
- inner_gate: bfloat16 [4096, 2048], P('sp', 'tp'), may hold values from -6 to 6
- conv_input: bfloat16 [4096, 2048], P('sp', 'tp'), may hold values from -6 to 6
- conv_taps: float32 [3, 2048], P(None, 'tp'), may hold values from -3.5 to 3.5
- out_proj: bfloat16 [2048, 2048], P('tp', 'sp'), may hold values from -0.125 to 0.125
Outputs:
- gate_weight_grad: bfloat16 [16, 1024, 2048], P('sp', 'tp')
- lin_weight_grad: bfloat16 [16, 1024, 2048], P('sp', 'tp')
- down_weight_grad: bfloat16 [16, 1024, 2048], P('sp', 'tp')
- out_proj_grad: float32 [2048, 2048], P('sp', 'tp')
- outer_gate_grad: bfloat16 [4096, 2048], P('sp', 'tp')
- inner_gate_grad: bfloat16 [4096, 2048], P('sp', 'tp')
- conv_input_grad: bfloat16 [4096, 2048], P('sp', 'tp')
The draws below stay inside these ranges and needn't reach their ends.
Inputs may be any that keep to these rules, and one draw needn't show every extreme that they name: `route_ids`: each row names 2 different experts. Among the rows of one device no expert is named more than 40 times, a bound that some block reaches.
All inputs are finite; a program needn't handle non-finite values.
Results may differ from the reference program's by a relative error of at most 0.015.
Values may be sent and summed in bfloat16 or wider, within the bound.
A program may use at most 64 MiB of HBM per device.

```python
import math
from functools import partial
import jax
import jax.numpy as jnp
import numpy as np
from jax import lax

D = 2048
FF = 1024
TOP = 2
TAPS = 3
TOK_DEV = 256
TOKENS = 4096
EXPERTS = 16
CAP = 40
FF_DEV = 512
N_SP = 16
N_TP = 2


def with_spikes(result, own_key, source, target, parts, factor):
    def block_of(dim):
        return (jnp.arange(result.shape[dim]) // (result.shape[dim] // parts)).reshape((-1,) + (1,) * (result.ndim - 1 - dim))

    first = jax.random.permutation(own_key, parts)[block_of(target)]
    other_side = (block_of(target) + parts // 2) % parts
    return jnp.where((block_of(source) == first) | (block_of(source) == other_side), factor * result, result)


def steps_of(own_key, dims, split, low, high):
    factor_of, own = 1.0, jax.random.fold_in(own_key, 6)
    for axis_at, shards_of in split:
        heights = jnp.exp(jax.random.uniform(jax.random.fold_in(own, axis_at), (shards_of,), jnp.float32, low / len(split), high / len(split)))
        factor_of = factor_of * jnp.repeat(heights, dims[axis_at] // shards_of).reshape([-1 if axis == axis_at else 1 for axis in range(len(dims))])
    return factor_of


def shared_out(rng, own, number, rows, number_of, top, limit, skew):
    sequence = jax.random.permutation(rng, number_of)
    packed, common = load_shares(number_of, rows * top, limit, skew, True), load_shares(number_of, rows * top, limit, skew, False)
    places = jnp.arange(number_of)

    def named(lengths, offset_by):
        used = int((lengths > 0).sum())
        fixed = max(1, used // 4)
        moved = fixed + (places - fixed + offset_by * (used - fixed)) % max(1, number_of - fixed)
        return jnp.zeros((number_of,), jnp.int32).at[sequence[jnp.where(places < fixed, places, moved)]].set(jnp.asarray(lengths, jnp.int32))

    lengths = jnp.where(number % 4 == 0, named(packed, number // 4), named(common, number - number // 4 - 1))
    mixed = jax.random.permutation(jax.random.fold_in(own, 3), number_of)
    source_of, receiver = mixed[0:number_of // 2 * 2:2], mixed[1:number_of // 2 * 2:2]
    margin = jnp.minimum(lengths[source_of] - 1, limit - lengths[receiver]) // 2
    margin = jnp.where((source_of == sequence[0]) | (receiver == sequence[0]) | (lengths[receiver] == 0), 0, jnp.maximum(margin, 0))
    moved = jax.random.randint(jax.random.fold_in(own, 4), (number_of // 2,), 0, 1 << 20) % (margin + 1)
    lengths = lengths.at[source_of].add(-moved).at[receiver].add(moved)
    items = jnp.searchsorted(jnp.cumsum(lengths), jnp.arange(rows * top), side="right").astype(jnp.int32)
    grid = items.reshape(top, rows).T
    grid = grid[jax.random.permutation(jax.random.fold_in(own, 1), rows)]
    offset_by = jax.random.randint(jax.random.fold_in(own, 2), (rows, 1), 0, top)
    return jnp.take_along_axis(grid, (jnp.arange(top)[None, :] + offset_by) % top, axis=1)


def load_shares(count, total, limit, skew, full):
    weights = [(1 << 20) // math.isqrt(rank ** skew) + 1 for rank in range(1, count + 1)]
    largest = limit if full else min(limit, max(-(-total // count), total * weights[0] // sum(weights)))
    least = 1 if total - largest >= count - 1 else 0
    given, rest = [largest] + [least] * (count - 1), total - largest - least * (count - 1)
    while rest > 0:
        free = [i for i in range(1, count) if given[i] < largest] or [i for i in range(1, count) if given[i] < limit]
        mass, left = sum([weights[i] for i in free]), rest
        for i in free:
            addition = min(limit - given[i], max(1, left * weights[i] // mass), rest)
            given[i] = given[i] + addition
            rest = rest - addition
    return np.array(given)


def noise(stream_key, shape, width, reach, shards=(), kind=jnp.bfloat16):
    gain = steps_of(stream_key, shape, shards, -0.22, 0.18) if shards else 1.0
    drawn = jax.random.normal(stream_key, shape, jnp.float32) * width * gain
    return jnp.minimum(jnp.maximum(drawn, -reach), reach).astype(kind)


def heavy_noise(key, dims, deviation, bound, shards, heavy, held_as=jnp.bfloat16):
    drawn = deviation * jax.random.normal(key, dims, jnp.float32)
    if shards:
        drawn = drawn * steps_of(key, dims, shards, -0.22, 0.18)
    return jnp.clip(with_spikes(drawn, jax.random.fold_in(key, 3), *heavy), -bound, bound).astype(held_as)


def setup_inputs(seed: int = 0) -> dict:
    keys = jax.random.split(jax.random.key(seed), 13)
    moe_input = noise(keys[0], (TOKENS, D), 1.0, 6.0, ((0, 16),))
    out_grad = heavy_noise(keys[1], (TOKENS, D), 0.05, 0.29882812, ((0, 16),), (0, 1, 16, 2.0))
    route_ids_keys = jax.random.split(jax.random.fold_in(keys[2], 1), TOKENS // TOK_DEV)
    route_ids_turns = jax.random.permutation(jax.random.fold_in(keys[2], 3), TOKENS // TOK_DEV)
    route_ids = jax.vmap(lambda own, number: shared_out(jax.random.fold_in(keys[2], 2), own, number, TOK_DEV, EXPERTS, TOP, CAP, 1))(route_ids_keys, route_ids_turns).reshape((TOKENS, TOP))
    route_weights = jnp.clip(0.2 + 0.8 * jax.random.uniform(keys[3], (TOKENS, TOP), jnp.float32) ** steps_of(keys[3], (TOKENS, TOP), ((0, 16),), -0.2, 0.2), 0.2, 1.0)
    gate_weight = noise(keys[4], (EXPERTS, FF, D), (D // 2) ** -0.5, 0.1875, ((0, 16), (1, 2)))
    lin_weight = noise(keys[5], (EXPERTS, FF, D), (D // 2) ** -0.5, 0.1875, ((0, 16), (1, 2)))
    down_weight = noise(keys[6], (EXPERTS, FF, D), FF ** -0.5, 0.1875, ((0, 16), (1, 2)))
    outer_gate = noise(keys[7], (TOKENS, D), 1.0, 6.0, ((0, 16), (1, 2)))
    inner_gate = noise(keys[8], (TOKENS, D), 1.0, 6.0, ((0, 16), (1, 2)))
    conv_input = noise(keys[9], (TOKENS, D), 1.0, 6.0, ((0, 16), (1, 2)))
    conv_taps = noise(keys[10], (TAPS, D), 3 ** -0.5, 3.5, ((1, 2),), jnp.float32)
    out_proj = noise(keys[11], (D, D), D ** -0.5, 0.125, ((0, 2), (1, 16)))
    return dict(moe_input=moe_input, out_grad=out_grad, route_ids=route_ids, route_weights=route_weights, gate_weight=gate_weight, lin_weight=lin_weight, down_weight=down_weight, outer_gate=outer_gate, inner_gate=inner_gate, conv_input=conv_input, conv_taps=conv_taps, out_proj=out_proj)


LIMIT = 7.0
ALPHA = 1.702


def slot_layout(flat_ids, experts, capacity):
    onehot = (flat_ids[:, None] == jnp.arange(experts, dtype=jnp.int32)[None, :]).astype(jnp.int32)
    before = (jnp.cumsum(onehot, axis=0) - onehot).astype(jnp.int32)
    slot_rank = jnp.sum(before * onehot, axis=1).astype(jnp.int32)
    position = (flat_ids.astype(jnp.int32) * capacity + slot_rank).astype(jnp.int32)
    pair_index = jnp.arange(flat_ids.shape[0], dtype=jnp.int32)
    source = jnp.full((experts * capacity,), -1, jnp.int32).at[position].set(pair_index)
    return position, source


def one_expert(operands):
    routed, cotan, gate_w, lin_w, down_w = operands
    routed = routed.astype(jnp.float32)
    cotan = cotan.astype(jnp.float32)
    gate_f = gate_w.astype(jnp.float32)
    lin_f = lin_w.astype(jnp.float32)
    gate_pre = jnp.dot(gate_f, routed.T)
    lin_pre = jnp.dot(lin_f, routed.T)
    gate_cut = jnp.minimum(gate_pre, LIMIT)
    lin_cut = jnp.clip(lin_pre, -LIMIT, LIMIT)
    sigma = jax.nn.sigmoid(ALPHA * gate_cut)
    act = (gate_cut * sigma * (lin_cut + 1.0)).astype(jnp.bfloat16)
    act_grad = jnp.dot(down_w.astype(jnp.float32), cotan.T)
    down_grad = jnp.dot(act.astype(jnp.float32), cotan).astype(jnp.bfloat16)
    slope = sigma * (1.0 + ALPHA * gate_cut * (1.0 - sigma))
    gate_cot = jnp.where(gate_pre < LIMIT, act_grad * (lin_cut + 1.0) * slope, 0.0).astype(jnp.bfloat16)
    lin_cot = jnp.where(jnp.abs(lin_pre) < LIMIT, act_grad * gate_cut * sigma, 0.0).astype(jnp.bfloat16)
    gate_grad = jnp.dot(gate_cot.astype(jnp.float32), routed).astype(jnp.bfloat16)
    lin_grad = jnp.dot(lin_cot.astype(jnp.float32), routed).astype(jnp.bfloat16)
    slots = routed.shape[0]
    gate_blocks = gate_cot.astype(jnp.float32).reshape(N_TP, FF_DEV, slots)
    lin_blocks = lin_cot.astype(jnp.float32).reshape(N_TP, FF_DEV, slots)
    partial_sums = jnp.einsum("bfr,bfd->brd", gate_blocks, gate_f.reshape(N_TP, FF_DEV, D))
    partial_sums = partial_sums + jnp.einsum("bfr,bfd->brd", lin_blocks, lin_f.reshape(N_TP, FF_DEV, D))
    partial_sums = partial_sums.astype(jnp.bfloat16).astype(jnp.float32)
    slot_grads = jnp.sum(partial_sums, axis=0).astype(jnp.bfloat16)
    return gate_grad, lin_grad, down_grad, slot_grads


def reference(moe_input, out_grad, route_ids, route_weights, gate_weight, lin_weight, down_weight, outer_gate, inner_gate, conv_input, conv_taps, out_proj):
    block_ids = route_ids.reshape(N_SP, TOK_DEV * TOP)
    position, source = jax.vmap(partial(slot_layout, experts=EXPERTS, capacity=CAP))(block_ids)
    source = source.reshape(N_SP, EXPERTS, CAP).transpose(1, 0, 2)
    block_base = (jnp.arange(N_SP, dtype=jnp.int32) * (TOK_DEV * TOP)).astype(jnp.int32)
    filled = source >= 0
    global_pair = jnp.where(filled, source + block_base[None, :, None], 0).astype(jnp.int32)
    filled = filled.reshape(EXPERTS, N_SP * CAP)
    global_pair = global_pair.reshape(EXPERTS, N_SP * CAP)
    token_row = (global_pair // TOP).astype(jnp.int32)
    routed_rows = jnp.where(filled[:, :, None], moe_input[token_row], jnp.zeros((), jnp.bfloat16))
    slot_weight = jnp.where(filled, route_weights.reshape(-1)[global_pair], 0.0)
    routed_grads = (slot_weight[:, :, None] * out_grad[token_row].astype(jnp.float32)).astype(jnp.bfloat16)
    gate_weight_grad, lin_weight_grad, down_weight_grad, slot_grads = lax.map(
        one_expert, (routed_rows, routed_grads, gate_weight, lin_weight, down_weight))
    slot_grads = slot_grads.reshape(EXPERTS, N_SP, CAP, D).transpose(1, 0, 2, 3).reshape(N_SP, EXPERTS * CAP, D)
    pair_grads = jax.vmap(lambda table, where_at: table[where_at])(slot_grads, position)
    row_grads = jnp.sum(pair_grads.astype(jnp.float32).reshape(TOKENS, TOP, D), axis=1).astype(jnp.bfloat16)
    stream_grad = (out_grad.astype(jnp.float32) + row_grads.astype(jnp.float32)).astype(jnp.bfloat16)
    conv_values = (inner_gate.astype(jnp.float32) * conv_input.astype(jnp.float32)).astype(jnp.bfloat16)
    padded = jnp.pad(conv_values.astype(jnp.float32), ((TAPS - 1, 0), (0, 0)))
    convolved = jnp.zeros((TOKENS, D), jnp.float32)
    for tap_index in range(TAPS):
        convolved = convolved + conv_taps[tap_index][None, :] * padded[tap_index:tap_index + TOKENS]
    mixed = (outer_gate.astype(jnp.float32) * convolved).astype(jnp.bfloat16)
    mixed_grad = jnp.dot(stream_grad, out_proj.T, preferred_element_type=jnp.float32)
    out_proj_grad = jnp.dot(stream_grad.T, mixed, preferred_element_type=jnp.float32)
    outer_gate_grad = (mixed_grad * convolved).astype(jnp.bfloat16)
    conv_cot = (mixed_grad * outer_gate.astype(jnp.float32)).astype(jnp.bfloat16)
    padded_cot = jnp.pad(conv_cot.astype(jnp.float32), ((0, TAPS - 1), (0, 0)))
    value_grad = jnp.zeros((TOKENS, D), jnp.float32)
    for tap_index in range(TAPS):
        first_row = TAPS - 1 - tap_index
        value_grad = value_grad + conv_taps[tap_index][None, :] * padded_cot[first_row:first_row + TOKENS]
    inner_gate_grad = (value_grad * conv_input.astype(jnp.float32)).astype(jnp.bfloat16)
    conv_input_grad = (value_grad * inner_gate.astype(jnp.float32)).astype(jnp.bfloat16)
    return (gate_weight_grad, lin_weight_grad, down_weight_grad, out_proj_grad, outer_gate_grad, inner_gate_grad, conv_input_grad)
```

```python
import functools

import jax
import jax.numpy as jnp
from jax import lax
from jax.experimental import pallas as pl
from jax.experimental.pallas import tpu as pltpu
from jax.sharding import PartitionSpec as P

LIMIT = 7.0
ALPHA = 1.702
BF16 = jnp.bfloat16
F32 = jnp.float32
MESH = pl.DeviceIdType.MESH
VMEM_LIMIT = 56 * 1024 * 1024
VMEM_SPEC = pl.BlockSpec(memory_space=pltpu.VMEM)


def from_behind(value, axis, by):
    count = lax.axis_size(axis)
    pairs = [(i, i + by) for i in range(count) if 0 <= i + by < count]
    return lax.ppermute(value, axis, pairs)


def remote(src, dst, send, recv, sp, tp):
    return pltpu.make_async_remote_copy(
        src_ref=src,
        dst_ref=dst,
        send_sem=send,
        recv_sem=recv,
        device_id=(sp, tp),
        device_id_type=MESH,
    )


def greet(peers):
    barrier = pltpu.get_barrier_semaphore()
    for peer in peers:
        pl.semaphore_signal(barrier, inc=1, device_id=peer, device_id_type=MESH)
    pl.semaphore_wait(barrier, len(peers))


def dispatch_kernel(
    n, p, rows_ref, grads_ref, routed, cotan, local_sem, send, recv, relay_send, relay_recv
):
    me, t = lax.axis_index("sp"), lax.axis_index("tp")
    width = rows_ref.shape[2]
    others = [lax.rem(me + k, n) for k in range(1, n)]
    sides = [lax.rem(t + k, p) for k in range(1, p)]
    greet([(o, t) for o in others] + [(me, s) for s in sides])
    mine = pl.ds(pl.multiple_of(t * width, width), width)
    pairs = ((rows_ref, routed), (grads_ref, cotan))
    started = []
    for a, (src, dst) in enumerate(pairs):
        own = pltpu.make_async_copy(src.at[me], dst.at[me, :, mine], local_sem.at[a])
        own.start()
        started.append(own)
    sends = []
    for a, (src, dst) in enumerate(pairs):
        for k in range(1, n):
            to = others[k - 1]
            copy = remote(
                src.at[to], dst.at[me, :, mine], send.at[a, k], recv.at[a, k], to, t
            )
            copy.start()
            sends.append(copy)
        for j in range(1, p):
            copy = remote(
                src.at[me],
                dst.at[me, :, mine],
                relay_send.at[a, 0, j],
                relay_recv.at[a, 0, j],
                me,
                sides[j - 1],
            )
            copy.start()
            sends.append(copy)
    for a, (src, dst) in enumerate(pairs):
        for k in range(1, n):
            frm = lax.rem(me - k + n, n)
            landed = dst.at[frm, :, mine]
            remote(src.at[frm], landed, send.at[a, k], recv.at[a, k], frm, t).wait_recv()
            for j in range(1, p):
                copy = remote(
                    landed, landed, relay_send.at[a, k, j], relay_recv.at[a, k, j], me, sides[j - 1]
                )
                copy.start()
                sends.append(copy)
    for own in started:
        own.wait()
    for a, (src, dst) in enumerate(pairs):
        for k in range(n):
            frm = lax.rem(me - k + n, n)
            for j in range(1, p):
                side = lax.rem(t - j + p, p)
                theirs = pl.ds(pl.multiple_of(side * width, width), width)
                landed = dst.at[frm, :, theirs]
                remote(
                    landed, landed, relay_send.at[a, k, j], relay_recv.at[a, k, j], me, side
                ).wait_recv()
    for copy in sends:
        copy.wait_send()


def dispatch(rows, grads, n, p):
    count, cap, width = rows.shape
    out = jax.ShapeDtypeStruct((n, cap, width * p), BF16)
    return pl.pallas_call(
        functools.partial(dispatch_kernel, n, p),
        out_shape=(out, out),
        in_specs=[VMEM_SPEC] * 2,
        out_specs=(VMEM_SPEC, VMEM_SPEC),
        scratch_shapes=[
            pltpu.SemaphoreType.DMA((2,)),
            pltpu.SemaphoreType.DMA((2, n)),
            pltpu.SemaphoreType.DMA((2, n)),
            pltpu.SemaphoreType.DMA((2, n, p)),
            pltpu.SemaphoreType.DMA((2, n, p)),
        ],
        compiler_params=pltpu.CompilerParams(
            collective_id=0, has_side_effects=True, vmem_limit_bytes=VMEM_LIMIT
        ),
    )(rows, grads)


def return_kernel(
    n,
    p,
    part,
    pick,
    full,
    beside,
    stage,
    back,
    total,
    side_send,
    side_recv,
    send,
    recv,
    row_send,
    row_recv,
):
    me, t = lax.axis_index("sp"), lax.axis_index("tp")
    width = stage.shape[2]
    others = [lax.rem(me + k, n) for k in range(1, n)]
    sides = [lax.rem(t + k, p) for k in range(1, p)]
    greet([(o, t) for o in others] + [(me, s) for s in sides])
    sends = []
    for k in list(range(1, n)) + [0]:
        to = lax.rem(me + k, n)
        for j in range(1, p):
            side = sides[j - 1]
            theirs = pl.ds(pl.multiple_of(side * width, width), width)
            copy = remote(
                part.at[to, :, theirs],
                beside.at[k, j],
                side_send.at[k, j],
                side_recv.at[k, j],
                me,
                side,
            )
            copy.start()
            sends.append(copy)
    mine = pl.ds(pl.multiple_of(t * width, width), width)
    for k in list(range(1, n)) + [0]:
        to = lax.rem(me + k, n)
        value = part[to, :, mine].astype(F32)
        for j in range(1, p):
            side = lax.rem(t - j + p, p)
            remote(
                part.at[to, :, mine], beside.at[k, j], side_send.at[k, j], side_recv.at[k, j], me, side
            ).wait_recv()
            value = value + beside[k, j].astype(F32)
        stage[k] = value.astype(BF16)
        if k > 0:
            copy = remote(stage.at[k], back.at[k], send.at[k], recv.at[k], to, t)
            copy.start()
            sends.append(copy)
    total[...] = jnp.dot(pick[me], stage[0], preferred_element_type=F32)
    for k in range(1, n):
        frm = lax.rem(me - k + n, n)
        remote(stage.at[k], back.at[k], send.at[k], recv.at[k], frm, t).wait_recv()
        total[...] += jnp.dot(pick[frm], back[k], preferred_element_type=F32)
    full[:, mine] = total[...].astype(BF16)
    for j in range(1, p):
        copy = remote(
            full.at[:, mine], full.at[:, mine], row_send.at[j], row_recv.at[j], me, sides[j - 1]
        )
        copy.start()
        sends.append(copy)
    for j in range(1, p):
        side = lax.rem(t - j + p, p)
        theirs = pl.ds(pl.multiple_of(side * width, width), width)
        remote(
            full.at[:, theirs], full.at[:, theirs], row_send.at[j], row_recv.at[j], me, side
        ).wait_recv()
    for copy in sends:
        copy.wait_send()


def return_rows(part, pick, n, p):
    count, cap, whole = part.shape
    tokens = pick.shape[1]
    width = whole // p
    return pl.pallas_call(
        functools.partial(return_kernel, n, p),
        out_shape=jax.ShapeDtypeStruct((tokens, whole), BF16),
        in_specs=[VMEM_SPEC] * 2,
        out_specs=VMEM_SPEC,
        scratch_shapes=[
            pltpu.VMEM((n, p, cap, width), BF16),
            pltpu.VMEM((n, cap, width), BF16),
            pltpu.VMEM((n, cap, width), BF16),
            pltpu.VMEM((tokens, width), F32),
            pltpu.SemaphoreType.DMA((n, p)),
            pltpu.SemaphoreType.DMA((n, p)),
            pltpu.SemaphoreType.DMA((n,)),
            pltpu.SemaphoreType.DMA((n,)),
            pltpu.SemaphoreType.DMA((p,)),
            pltpu.SemaphoreType.DMA((p,)),
        ],
        compiler_params=pltpu.CompilerParams(
            collective_id=1, has_side_effects=True, vmem_limit_bytes=VMEM_LIMIT
        ),
    )(part, pick)


def scatter_kernel(
    m,
    chunks,
    terms,
    out,
    core_in,
    core_sum,
    pair_in,
    pair_sum,
    far_in,
    core_send,
    core_recv,
    pair_send,
    pair_recv,
    far_send,
    far_recv,
):
    me, t = lax.axis_index("sp"), lax.axis_index("tp")
    c = lax.rem(me, 2)
    x = lax.rem(me // 2, 2)
    z = me // 4
    core_peer = me + 1 - 2 * c
    pair_peer = me + 2 - 4 * x
    far = [lax.rem(z + k, m) * 4 + x * 2 + c for k in range(1, m)]
    back = [lax.rem(z - k + m, m) * 4 + x * 2 + c for k in range(1, m)]
    greet([(core_peer, t), (pair_peer, t)] + [(f, t) for f in far])
    rows = terms.shape[3] // chunks
    cuts = [pl.ds(i * rows, rows) for i in range(chunks)]
    sends = []
    order = [lax.rem(z + k, m) for k in list(range(1, m)) + [0]]
    for i, cut in enumerate(cuts):
        for q in range(2):
            xx = 1 - x if q == 0 else x
            for k in range(m):
                copy = remote(
                    terms.at[order[k], xx, 1 - c, cut],
                    core_in.at[i, q, k],
                    core_send.at[i, q, k],
                    core_recv.at[i, q, k],
                    core_peer,
                    t,
                )
                copy.start()
                sends.append(copy)
    for i, cut in enumerate(cuts):
        for q in range(2):
            xx = 1 - x if q == 0 else x
            for k in range(m):
                remote(
                    terms.at[order[k], xx, 1 - c, cut],
                    core_in.at[i, q, k],
                    core_send.at[i, q, k],
                    core_recv.at[i, q, k],
                    core_peer,
                    t,
                ).wait_recv()
                core_sum[i, q, k] = (
                    terms[order[k], xx, c, cut].astype(F32) + core_in[i, q, k].astype(F32)
                ).astype(BF16)
                if q == 0:
                    copy = remote(
                        core_sum.at[i, 0, k],
                        pair_in.at[i, k],
                        pair_send.at[i, k],
                        pair_recv.at[i, k],
                        pair_peer,
                        t,
                    )
                    copy.start()
                    sends.append(copy)
    for i, cut in enumerate(cuts):
        for k in range(m):
            remote(
                core_sum.at[i, 0, k],
                pair_in.at[i, k],
                pair_send.at[i, k],
                pair_recv.at[i, k],
                pair_peer,
                t,
            ).wait_recv()
            value = core_sum[i, 1, k].astype(F32) + pair_in[i, k].astype(F32)
            if k < m - 1:
                pair_sum[i, k] = value.astype(BF16)
                copy = remote(
                    pair_sum.at[i, k],
                    far_in.at[i, k],
                    far_send.at[i, k],
                    far_recv.at[i, k],
                    far[k],
                    t,
                )
                copy.start()
                sends.append(copy)
            else:
                out[cut] = value
    for i, cut in enumerate(cuts):
        for k in range(m - 1):
            remote(
                pair_sum.at[i, k],
                far_in.at[i, k],
                far_send.at[i, k],
                far_recv.at[i, k],
                back[k],
                t,
            ).wait_recv()
            out[cut] += far_in[i, k].astype(F32)
    for copy in sends:
        copy.wait_send()


def scatter_sum(terms, n):
    total, width = terms.shape
    rows = total // n
    m = n // 4
    chunks = 4
    part = rows // chunks
    return pl.pallas_call(
        functools.partial(scatter_kernel, m, chunks),
        out_shape=jax.ShapeDtypeStruct((rows, width), F32),
        in_specs=[VMEM_SPEC],
        out_specs=VMEM_SPEC,
        scratch_shapes=[
            pltpu.VMEM((chunks, 2, m, part, width), BF16),
            pltpu.VMEM((chunks, 2, m, part, width), BF16),
            pltpu.VMEM((chunks, m, part, width), BF16),
            pltpu.VMEM((chunks, m, part, width), BF16),
            pltpu.VMEM((chunks, m, part, width), BF16),
            pltpu.SemaphoreType.DMA((chunks, 2, m)),
            pltpu.SemaphoreType.DMA((chunks, 2, m)),
            pltpu.SemaphoreType.DMA((chunks, m)),
            pltpu.SemaphoreType.DMA((chunks, m)),
            pltpu.SemaphoreType.DMA((chunks, m)),
            pltpu.SemaphoreType.DMA((chunks, m)),
        ],
        compiler_params=pltpu.CompilerParams(
            collective_id=2, has_side_effects=True, vmem_limit_bytes=VMEM_LIMIT
        ),
    )(terms.reshape(m, 2, 2, rows, width))


def slot_positions(route_ids, experts, capacity):
    tokens, top_count = route_ids.shape
    flat = route_ids.reshape(-1)
    onehot = flat[:, None] == jnp.arange(experts, dtype=jnp.int32)[None, :]
    index = jnp.arange(flat.shape[0], dtype=jnp.int32)
    earlier = (index[:, None] > index[None, :]).astype(BF16)
    before = jnp.dot(earlier, onehot.astype(BF16), preferred_element_type=F32)
    slot_rank = jnp.sum(jnp.where(onehot, before, 0.0), axis=1).astype(jnp.int32)
    return (flat * capacity + slot_rank).reshape(tokens, top_count)


def local(
    moe_input,
    out_grad,
    route_ids,
    route_weights,
    gate_weight,
    lin_weight,
    down_weight,
    outer_gate,
    inner_gate,
    conv_input,
    conv_taps,
    out_proj,
):
    n = lax.axis_size("sp")
    p = lax.axis_size("tp")
    local_experts = gate_weight.shape[0]
    assert local_experts == 1
    experts = local_experts * n
    tokens, top_count = route_ids.shape
    width = moe_input.shape[1]
    width_dev = width // p
    capacity = 5 * tokens // (2 * experts)
    capacity = -(-capacity // 8) * 8
    slots = experts * capacity
    position = slot_positions(route_ids, experts, capacity)
    slot_index = jnp.arange(slots, dtype=jnp.int32)
    hits = [position[:, k][None, :] == slot_index[:, None] for k in range(top_count)]
    taken = functools.reduce(jnp.logical_or, hits)
    slot_weight = sum(
        jnp.sum(jnp.where(hits[k], route_weights[:, k][None, :], 0.0), axis=1)
        for k in range(top_count)
    )
    select = taken.astype(BF16)
    column_start = lax.axis_index("tp") * width_dev
    part_rows = lax.dynamic_slice_in_dim(moe_input, column_start, width_dev, 1)
    part_grads = lax.dynamic_slice_in_dim(out_grad, column_start, width_dev, 1)
    send_rows = jnp.dot(select, part_rows, preferred_element_type=F32).astype(BF16)
    send_grads = (
        slot_weight[:, None] * jnp.dot(select, part_grads, preferred_element_type=F32)
    ).astype(BF16)
    routed, cotan = dispatch(
        send_rows.reshape(experts, capacity, width_dev),
        send_grads.reshape(experts, capacity, width_dev),
        n,
        p,
    )
    routed = routed.reshape(slots, width)
    cotan = cotan.reshape(slots, width)
    gate_w, lin_w, down_w = gate_weight[0], lin_weight[0], down_weight[0]

    def product(a, b, left, right):
        return lax.dot_general(a, b, (((left,), (right,)), ((), ())), preferred_element_type=F32)

    gate_pre = product(gate_w, routed, 1, 1)
    lin_pre = product(lin_w, routed, 1, 1)
    act_grad = product(down_w, cotan, 1, 1)
    gate_cut = jnp.minimum(gate_pre, LIMIT)
    lin_cut = jnp.clip(lin_pre, -LIMIT, LIMIT)
    sigma = jax.nn.sigmoid(ALPHA * gate_cut)
    act = (gate_cut * sigma * (lin_cut + 1.0)).astype(BF16)
    slope = sigma * (1.0 + ALPHA * gate_cut * (1.0 - sigma))
    gate_cot = jnp.where(gate_pre < LIMIT, act_grad * (lin_cut + 1.0) * slope, 0.0).astype(BF16)
    lin_cot = jnp.where(jnp.abs(lin_pre) < LIMIT, act_grad * gate_cut * sigma, 0.0).astype(BF16)
    input_part = (product(gate_cot, gate_w, 0, 0) + product(lin_cot, lin_w, 0, 0)).astype(BF16)
    down_grad = product(act, cotan, 1, 0).astype(BF16)[None]
    gate_grad = product(gate_cot, routed, 1, 0).astype(BF16)[None]
    lin_grad = product(lin_cot, routed, 1, 0).astype(BF16)[None]

    expert_slot = slot_index.reshape(experts, 1, capacity)
    pick = functools.reduce(
        jnp.logical_or,
        [position[:, k][None, :, None] == expert_slot for k in range(top_count)],
    ).astype(BF16)
    full_rows = return_rows(input_part.reshape(n, capacity, width), pick, n, p)
    stream_grad = (out_grad.astype(F32) + full_rows.astype(F32)).astype(BF16)

    tap_count = conv_taps.shape[0]
    conv_values = (inner_gate.astype(F32) * conv_input.astype(F32)).astype(BF16)
    prior_rows = from_behind(conv_values[tokens - (tap_count - 1) :], "sp", 1)
    extended = jnp.concatenate([prior_rows, conv_values], axis=0).astype(F32)
    convolved = jnp.zeros((tokens, width_dev), F32)
    for tap_index in range(tap_count):
        convolved = (
            convolved + conv_taps[tap_index][None, :] * extended[tap_index : tap_index + tokens]
        )
    mixed = (outer_gate.astype(F32) * convolved).astype(BF16)
    proj = lax.all_gather(out_proj, "sp", axis=1, tiled=True)
    mixed_grad = product(stream_grad, proj, 1, 1)
    out_proj_grad = scatter_sum(product(stream_grad, mixed, 0, 0).astype(BF16), n)
    outer_gate_grad = (mixed_grad * convolved).astype(BF16)
    conv_cot = (mixed_grad * outer_gate.astype(F32)).astype(BF16)
    later_rows = from_behind(conv_cot[: tap_count - 1], "sp", -1)
    extended_cot = jnp.concatenate([conv_cot, later_rows], axis=0).astype(F32)
    value_grad = jnp.zeros((tokens, width_dev), F32)
    for tap_index in range(tap_count):
        first_row = tap_count - 1 - tap_index
        value_grad = (
            value_grad
            + conv_taps[tap_index][None, :] * extended_cot[first_row : first_row + tokens]
        )
    inner_gate_grad = (value_grad * conv_input.astype(F32)).astype(BF16)
    conv_input_grad = (value_grad * inner_gate.astype(F32)).astype(BF16)
    return (
        gate_grad,
        lin_grad,
        down_grad,
        out_proj_grad,
        outer_gate_grad,
        inner_gate_grad,
        conv_input_grad,
    )


def solution(mesh):
    placed = (
        P("sp", None),
        P("sp", None),
        P("sp", None),
        P("sp", None),
        P("sp", "tp", None),
        P("sp", "tp", None),
        P("sp", "tp", None),
        P("sp", "tp"),
        P("sp", "tp"),
        P("sp", "tp"),
        P(None, "tp"),
        P("tp", "sp"),
    )
    return jax.shard_map(
        local,
        mesh=mesh,
        in_specs=placed,
        out_specs=(
            P("sp", "tp", None),
            P("sp", "tp", None),
            P("sp", "tp", None),
            P("sp", "tp"),
            P("sp", "tp"),
            P("sp", "tp"),
            P("sp", "tp"),
        ),
        check_vma=False,
    )
```

```python
import functools

import jax
import jax.numpy as jnp
from jax import lax
from jax.experimental import pallas as pl
from jax.experimental.pallas import tpu as pltpu
from jax.sharding import PartitionSpec as P

LIMIT = 7.0
ALPHA = 1.702
BF16 = jnp.bfloat16
F32 = jnp.float32
MESH = pl.DeviceIdType.MESH
VMEM_LIMIT = 56 * 1024 * 1024
VMEM_SPEC = pl.BlockSpec(memory_space=pltpu.VMEM)


def from_behind(value, axis, by):
    count = lax.axis_size(axis)
    pairs = [(i, i + by) for i in range(count) if 0 <= i + by < count]
    return lax.ppermute(value, axis, pairs)


def remote(src, dst, send, recv, sp, tp):
    return pltpu.make_async_remote_copy(
        src_ref=src,
        dst_ref=dst,
        send_sem=send,
        recv_sem=recv,
        device_id=(sp, tp),
        device_id_type=MESH,
    )


def greet(peers):
    barrier = pltpu.get_barrier_semaphore()
    for peer in peers:
        pl.semaphore_signal(barrier, inc=1, device_id=peer, device_id_type=MESH)
    pl.semaphore_wait(barrier, len(peers))


def ring_order(m):
    far = sorted(range(1, m), key=lambda d: (abs(2 * d - m), d))
    return [(d, j) for j in range(4) for d in far], [(0, j) for j in range(1, 4)]


def to_peer(me, m, d, j):
    return lax.rem(me // 4 + d, m) * 4 + lax.rem(lax.rem(me, 4) + j, 4)


def from_peer(me, m, d, j):
    return lax.rem(me // 4 - d + m, m) * 4 + lax.rem(lax.rem(me, 4) - j + 4, 4)


def dispatch_kernel(
    n, p, rows_ref, grads_ref, routed, cotan, local_sem, send, recv, relay_send, relay_recv
):
    me, t = lax.axis_index("sp"), lax.axis_index("tp")
    m = n // 4
    width = rows_ref.shape[2] // p
    far, near = ring_order(m)
    sides = [lax.rem(t + k, p) for k in range(1, p)]
    greet([(to_peer(me, m, d, j), t) for d, j in far + near] + [(me, s) for s in sides])
    mine = pl.ds(pl.multiple_of(t * width, width), width)
    pairs = ((rows_ref, routed), (grads_ref, cotan))
    sends = []
    started = []
    for a, (src, dst) in enumerate(pairs):
        for d, j in far:
            to = to_peer(me, m, d, j)
            i = d * 4 + j
            copy = remote(
                src.at[to, :, mine], dst.at[me, :, mine], send.at[a, i], recv.at[a, i], to, t
            )
            copy.start()
            sends.append(copy)
        for d, j in near:
            to = to_peer(me, m, d, j)
            i = d * 4 + j
            copy = remote(src.at[to], dst.at[me], send.at[a, i], recv.at[a, i], to, t)
            copy.start()
            sends.append(copy)
        own = pltpu.make_async_copy(src.at[me], dst.at[me], local_sem.at[a])
        own.start()
        started.append(own)
    for a, (src, dst) in enumerate(pairs):
        for d, j in far:
            frm = from_peer(me, m, d, j)
            i = d * 4 + j
            landed = dst.at[frm, :, mine]
            remote(
                src.at[frm, :, mine], landed, send.at[a, i], recv.at[a, i], frm, t
            ).wait_recv()
            for k in range(1, p):
                copy = remote(
                    landed, landed, relay_send.at[a, i, k], relay_recv.at[a, i, k], me, sides[k - 1]
                )
                copy.start()
                sends.append(copy)
    for own in started:
        own.wait()
    for a, (src, dst) in enumerate(pairs):
        for d, j in near:
            frm = from_peer(me, m, d, j)
            i = d * 4 + j
            remote(src.at[frm], dst.at[frm], send.at[a, i], recv.at[a, i], frm, t).wait_recv()
        for d, j in far:
            frm = from_peer(me, m, d, j)
            i = d * 4 + j
            for k in range(1, p):
                side = lax.rem(t - k + p, p)
                theirs = pl.ds(pl.multiple_of(side * width, width), width)
                landed = dst.at[frm, :, theirs]
                remote(
                    landed, landed, relay_send.at[a, i, k], relay_recv.at[a, i, k], me, side
                ).wait_recv()
    for copy in sends:
        copy.wait_send()


def dispatch(rows, grads, n, p):
    count, cap, width = rows.shape
    out = jax.ShapeDtypeStruct((n, cap, width), BF16)
    return pl.pallas_call(
        functools.partial(dispatch_kernel, n, p),
        out_shape=(out, out),
        in_specs=[VMEM_SPEC] * 2,
        out_specs=(VMEM_SPEC, VMEM_SPEC),
        scratch_shapes=[
            pltpu.SemaphoreType.DMA((2,)),
            pltpu.SemaphoreType.DMA((2, n)),
            pltpu.SemaphoreType.DMA((2, n)),
            pltpu.SemaphoreType.DMA((2, n, p)),
            pltpu.SemaphoreType.DMA((2, n, p)),
        ],
        compiler_params=pltpu.CompilerParams(
            collective_id=0, has_side_effects=True, vmem_limit_bytes=VMEM_LIMIT
        ),
    )(rows, grads)


def return_kernel(
    n,
    p,
    cuts,
    part,
    pick,
    full,
    beside,
    stage,
    back,
    total,
    side_send,
    side_recv,
    send,
    recv,
    row_send,
    row_recv,
):
    me, t = lax.axis_index("sp"), lax.axis_index("tp")
    m = n // 4
    width = full.shape[1] // p
    span = width // cuts
    far, near = ring_order(m)
    every = far + near + [(0, 0)]
    sides = [lax.rem(t + k, p) for k in range(1, p)]
    greet([(to_peer(me, m, d, j), t) for d, j in far + near] + [(me, s) for s in sides])

    def columns(side, q):
        return pl.ds(pl.multiple_of(side * width + q * span, span), span)

    sends = []
    for q in range(cuts):
        for d, j in every:
            to = to_peer(me, m, d, j)
            i = d * 4 + j
            for k in range(1, p):
                side = sides[k - 1]
                copy = remote(
                    part.at[to, :, columns(side, q)],
                    beside.at[q, i, k],
                    side_send.at[q, i, k],
                    side_recv.at[q, i, k],
                    me,
                    side,
                )
                copy.start()
                sends.append(copy)
    def add_and_send(q, d, j):
        mine = columns(t, q)
        to = to_peer(me, m, d, j)
        i = d * 4 + j
        value = part[to, :, mine].astype(F32)
        for k in range(1, p):
            side = lax.rem(t - k + p, p)
            remote(
                part.at[to, :, mine],
                beside.at[q, i, k],
                side_send.at[q, i, k],
                side_recv.at[q, i, k],
                me,
                side,
            ).wait_recv()
            value = value + beside[q, i, k].astype(F32)
        stage[q, i] = value.astype(BF16)
        if i > 0:
            copy = remote(stage.at[q, i], back.at[q, i], send.at[q, i], recv.at[q, i], to, t)
            copy.start()
            sends.append(copy)

    def take(q, d, j):
        frm = from_peer(me, m, d, j)
        i = d * 4 + j
        remote(stage.at[q, i], back.at[q, i], send.at[q, i], recv.at[q, i], frm, t).wait_recv()
        total[...] += jnp.dot(pick[frm], back[q, i], preferred_element_type=F32)

    for q in range(cuts + 1):
        if q > 0:
            total[...] = jnp.dot(pick[me], stage[q - 1, 0], preferred_element_type=F32)
        for d, j in every:
            if q < cuts:
                add_and_send(q, d, j)
            if q > 0 and d * 4 + j > 0:
                take(q - 1, d, j)
        if q > 0:
            mine = columns(t, q - 1)
            full[:, mine] = total[...].astype(BF16)
            for k in range(1, p):
                copy = remote(
                    full.at[:, mine],
                    full.at[:, mine],
                    row_send.at[q - 1, k],
                    row_recv.at[q - 1, k],
                    me,
                    sides[k - 1],
                )
                copy.start()
                sends.append(copy)
    for q in range(cuts):
        for k in range(1, p):
            side = lax.rem(t - k + p, p)
            theirs = columns(side, q)
            remote(
                full.at[:, theirs], full.at[:, theirs], row_send.at[q, k], row_recv.at[q, k], me, side
            ).wait_recv()
    for copy in sends:
        copy.wait_send()


def return_rows(part, pick, n, p):
    count, cap, whole = part.shape
    tokens = pick.shape[1]
    width = whole // p
    cuts = 2 if width % 256 == 0 else 1
    span = width // cuts
    return pl.pallas_call(
        functools.partial(return_kernel, n, p, cuts),
        out_shape=jax.ShapeDtypeStruct((tokens, whole), BF16),
        in_specs=[VMEM_SPEC] * 2,
        out_specs=VMEM_SPEC,
        scratch_shapes=[
            pltpu.VMEM((cuts, n, p, cap, span), BF16),
            pltpu.VMEM((cuts, n, cap, span), BF16),
            pltpu.VMEM((cuts, n, cap, span), BF16),
            pltpu.VMEM((tokens, span), F32),
            pltpu.SemaphoreType.DMA((cuts, n, p)),
            pltpu.SemaphoreType.DMA((cuts, n, p)),
            pltpu.SemaphoreType.DMA((cuts, n)),
            pltpu.SemaphoreType.DMA((cuts, n)),
            pltpu.SemaphoreType.DMA((cuts, p)),
            pltpu.SemaphoreType.DMA((cuts, p)),
        ],
        compiler_params=pltpu.CompilerParams(
            collective_id=1, has_side_effects=True, vmem_limit_bytes=VMEM_LIMIT
        ),
    )(part, pick)


def scatter_kernel(
    m,
    chunks,
    terms,
    out,
    core_in,
    core_sum,
    pair_in,
    pair_sum,
    far_in,
    core_send,
    core_recv,
    pair_send,
    pair_recv,
    far_send,
    far_recv,
):
    me, t = lax.axis_index("sp"), lax.axis_index("tp")
    c = lax.rem(me, 2)
    x = lax.rem(me // 2, 2)
    z = me // 4
    core_peer = me + 1 - 2 * c
    pair_peer = me + 2 - 4 * x
    far = [lax.rem(z + k, m) * 4 + x * 2 + c for k in range(1, m)]
    back = [lax.rem(z - k + m, m) * 4 + x * 2 + c for k in range(1, m)]
    greet([(core_peer, t), (pair_peer, t)] + [(f, t) for f in far])
    rows = terms.shape[3] // chunks
    cuts = [pl.ds(i * rows, rows) for i in range(chunks)]
    sends = []
    order = [lax.rem(z + k, m) for k in list(range(1, m)) + [0]]
    for i, cut in enumerate(cuts):
        for q in range(2):
            xx = 1 - x if q == 0 else x
            for k in range(m):
                copy = remote(
                    terms.at[order[k], xx, 1 - c, cut],
                    core_in.at[i, q, k],
                    core_send.at[i, q, k],
                    core_recv.at[i, q, k],
                    core_peer,
                    t,
                )
                copy.start()
                sends.append(copy)
    for i, cut in enumerate(cuts):
        for q in range(2):
            xx = 1 - x if q == 0 else x
            for k in range(m):
                remote(
                    terms.at[order[k], xx, 1 - c, cut],
                    core_in.at[i, q, k],
                    core_send.at[i, q, k],
                    core_recv.at[i, q, k],
                    core_peer,
                    t,
                ).wait_recv()
                core_sum[i, q, k] = (
                    terms[order[k], xx, c, cut].astype(F32) + core_in[i, q, k].astype(F32)
                ).astype(BF16)
                if q == 0:
                    copy = remote(
                        core_sum.at[i, 0, k],
                        pair_in.at[i, k],
                        pair_send.at[i, k],
                        pair_recv.at[i, k],
                        pair_peer,
                        t,
                    )
                    copy.start()
                    sends.append(copy)
    for i, cut in enumerate(cuts):
        for k in range(m):
            remote(
                core_sum.at[i, 0, k],
                pair_in.at[i, k],
                pair_send.at[i, k],
                pair_recv.at[i, k],
                pair_peer,
                t,
            ).wait_recv()
            value = core_sum[i, 1, k].astype(F32) + pair_in[i, k].astype(F32)
            if k < m - 1:
                pair_sum[i, k] = value.astype(BF16)
                copy = remote(
                    pair_sum.at[i, k],
                    far_in.at[i, k],
                    far_send.at[i, k],
                    far_recv.at[i, k],
                    far[k],
                    t,
                )
                copy.start()
                sends.append(copy)
            else:
                out[cut] = value
    for i, cut in enumerate(cuts):
        for k in range(m - 1):
            remote(
                pair_sum.at[i, k],
                far_in.at[i, k],
                far_send.at[i, k],
                far_recv.at[i, k],
                back[k],
                t,
            ).wait_recv()
            out[cut] += far_in[i, k].astype(F32)
    for copy in sends:
        copy.wait_send()


def scatter_sum(terms, n):
    total, width = terms.shape
    rows = total // n
    m = n // 4
    chunks = 4
    part = rows // chunks
    return pl.pallas_call(
        functools.partial(scatter_kernel, m, chunks),
        out_shape=jax.ShapeDtypeStruct((rows, width), F32),
        in_specs=[VMEM_SPEC],
        out_specs=VMEM_SPEC,
        scratch_shapes=[
            pltpu.VMEM((chunks, 2, m, part, width), BF16),
            pltpu.VMEM((chunks, 2, m, part, width), BF16),
            pltpu.VMEM((chunks, m, part, width), BF16),
            pltpu.VMEM((chunks, m, part, width), BF16),
            pltpu.VMEM((chunks, m, part, width), BF16),
            pltpu.SemaphoreType.DMA((chunks, 2, m)),
            pltpu.SemaphoreType.DMA((chunks, 2, m)),
            pltpu.SemaphoreType.DMA((chunks, m)),
            pltpu.SemaphoreType.DMA((chunks, m)),
            pltpu.SemaphoreType.DMA((chunks, m)),
            pltpu.SemaphoreType.DMA((chunks, m)),
        ],
        compiler_params=pltpu.CompilerParams(
            collective_id=2, has_side_effects=True, vmem_limit_bytes=VMEM_LIMIT
        ),
    )(terms.reshape(m, 2, 2, rows, width))


def slot_positions(route_ids, experts, capacity):
    tokens, top_count = route_ids.shape
    flat = route_ids.reshape(-1)
    onehot = flat[:, None] == jnp.arange(experts, dtype=jnp.int32)[None, :]
    index = jnp.arange(flat.shape[0], dtype=jnp.int32)
    earlier = (index[:, None] > index[None, :]).astype(BF16)
    before = jnp.dot(earlier, onehot.astype(BF16), preferred_element_type=F32)
    slot_rank = jnp.sum(jnp.where(onehot, before, 0.0), axis=1).astype(jnp.int32)
    return (flat * capacity + slot_rank).reshape(tokens, top_count)


def local(
    moe_input,
    out_grad,
    route_ids,
    route_weights,
    gate_weight,
    lin_weight,
    down_weight,
    outer_gate,
    inner_gate,
    conv_input,
    conv_taps,
    out_proj,
):
    n = lax.axis_size("sp")
    p = lax.axis_size("tp")
    local_experts = gate_weight.shape[0]
    assert local_experts == 1
    experts = local_experts * n
    tokens, top_count = route_ids.shape
    width = moe_input.shape[1]
    width_dev = width // p
    capacity = 5 * tokens // (2 * experts)
    capacity = -(-capacity // 8) * 8
    slots = experts * capacity
    position = slot_positions(route_ids, experts, capacity)
    slot_index = jnp.arange(slots, dtype=jnp.int32)
    hits = [position[:, k][None, :] == slot_index[:, None] for k in range(top_count)]
    taken = functools.reduce(jnp.logical_or, hits)
    slot_weight = sum(
        jnp.sum(jnp.where(hits[k], route_weights[:, k][None, :], 0.0), axis=1)
        for k in range(top_count)
    )
    select = taken.astype(BF16)
    send_rows = jnp.dot(select, moe_input, preferred_element_type=F32).astype(BF16)
    send_grads = (
        slot_weight[:, None] * jnp.dot(select, out_grad, preferred_element_type=F32)
    ).astype(BF16)
    routed, cotan = dispatch(
        send_rows.reshape(experts, capacity, width),
        send_grads.reshape(experts, capacity, width),
        n,
        p,
    )
    routed, cotan, out_proj = lax.optimization_barrier((routed, cotan, out_proj))
    routed = routed.reshape(slots, width)
    cotan = cotan.reshape(slots, width)
    gate_w, lin_w, down_w = gate_weight[0], lin_weight[0], down_weight[0]

    def product(a, b, left, right):
        return lax.dot_general(a, b, (((left,), (right,)), ((), ())), preferred_element_type=F32)

    gate_pre = product(gate_w, routed, 1, 1)
    lin_pre = product(lin_w, routed, 1, 1)
    act_grad = product(down_w, cotan, 1, 1)
    gate_cut = jnp.minimum(gate_pre, LIMIT)
    lin_cut = jnp.clip(lin_pre, -LIMIT, LIMIT)
    sigma = jax.nn.sigmoid(ALPHA * gate_cut)
    act = (gate_cut * sigma * (lin_cut + 1.0)).astype(BF16)
    slope = sigma * (1.0 + ALPHA * gate_cut * (1.0 - sigma))
    gate_cot = jnp.where(gate_pre < LIMIT, act_grad * (lin_cut + 1.0) * slope, 0.0).astype(BF16)
    lin_cot = jnp.where(jnp.abs(lin_pre) < LIMIT, act_grad * gate_cut * sigma, 0.0).astype(BF16)
    input_part = (product(gate_cot, gate_w, 0, 0) + product(lin_cot, lin_w, 0, 0)).astype(BF16)
    down_grad = product(act, cotan, 1, 0).astype(BF16)[None]
    gate_grad = product(gate_cot, routed, 1, 0).astype(BF16)[None]
    lin_grad = product(lin_cot, routed, 1, 0).astype(BF16)[None]

    expert_slot = slot_index.reshape(experts, 1, capacity)
    pick = functools.reduce(
        jnp.logical_or,
        [position[:, k][None, :, None] == expert_slot for k in range(top_count)],
    ).astype(BF16)
    full_rows = return_rows(input_part.reshape(n, capacity, width), pick, n, p)
    stream_grad = (out_grad.astype(F32) + full_rows.astype(F32)).astype(BF16)

    tap_count = conv_taps.shape[0]
    conv_values = (inner_gate.astype(F32) * conv_input.astype(F32)).astype(BF16)
    prior_rows = from_behind(conv_values[tokens - (tap_count - 1) :], "sp", 1)
    extended = jnp.concatenate([prior_rows, conv_values], axis=0).astype(F32)
    convolved = jnp.zeros((tokens, width_dev), F32)
    for tap_index in range(tap_count):
        convolved = (
            convolved + conv_taps[tap_index][None, :] * extended[tap_index : tap_index + tokens]
        )
    mixed = (outer_gate.astype(F32) * convolved).astype(BF16)
    proj = lax.all_gather(out_proj, "sp", axis=1, tiled=True)
    mixed_grad = product(stream_grad, proj, 1, 1)
    out_proj_grad = scatter_sum(product(stream_grad, mixed, 0, 0).astype(BF16), n)
    outer_gate_grad = (mixed_grad * convolved).astype(BF16)
    conv_cot = (mixed_grad * outer_gate.astype(F32)).astype(BF16)
    later_rows = from_behind(conv_cot[: tap_count - 1], "sp", -1)
    extended_cot = jnp.concatenate([conv_cot, later_rows], axis=0).astype(F32)
    value_grad = jnp.zeros((tokens, width_dev), F32)
    for tap_index in range(tap_count):
        first_row = tap_count - 1 - tap_index
        value_grad = (
            value_grad
            + conv_taps[tap_index][None, :] * extended_cot[first_row : first_row + tokens]
        )
    inner_gate_grad = (value_grad * conv_input.astype(F32)).astype(BF16)
    conv_input_grad = (value_grad * inner_gate.astype(F32)).astype(BF16)
    return (
        gate_grad,
        lin_grad,
        down_grad,
        out_proj_grad,
        outer_gate_grad,
        inner_gate_grad,
        conv_input_grad,
    )


def solution(mesh):
    placed = (
        P("sp", None),
        P("sp", None),
        P("sp", None),
        P("sp", None),
        P("sp", "tp", None),
        P("sp", "tp", None),
        P("sp", "tp", None),
        P("sp", "tp"),
        P("sp", "tp"),
        P("sp", "tp"),
        P(None, "tp"),
        P("tp", "sp"),
    )
    return jax.shard_map(
        local,
        mesh=mesh,
        in_specs=placed,
        out_specs=(
            P("sp", "tp", None),
            P("sp", "tp", None),
            P("sp", "tp", None),
            P("sp", "tp"),
            P("sp", "tp"),
            P("sp", "tp"),
            P("sp", "tp"),
        ),
        check_vma=False,
    )
```
